32 devices in a mesh: grp: 2 (over x), ep: 4 (over y, core), tp: 4 (over z).
Axes of the slice: x: 2, y: 2, z: 4, core: 2. Of those that a mesh axis runs over, the one named last changes fastest.
Arguments:
- tokens: bfloat16 [4096, 1024], P(('grp', 'ep', 'tp')), parts along dimension 0, may hold values from -6 to 6
- norm_gain: float32 [1024], replicated, may hold values from 0.1 to 1.9
- gate_weight: bfloat16 [4, 1024, 3584], P('ep', None, 'tp'), may hold values from -0.1875 to 0.1875
- up_weight: bfloat16 [4, 1024, 3584], P('ep', None, 'tp'), may hold values from -0.1875 to 0.1875
- down_weight: bfloat16 [4, 3584, 1024], P('ep', 'tp'), may hold values from -0.09375 to 0.09375
- expert_ids: int32 [4096, 2], P(('grp', 'ep')), parts along dimension 0, may hold values from 0 to 3, all different within a row; in each aligned block of 128 rows (0 to 127, 128 to 255, ...) at most 80 rows name the same one
- route_weight: float32 [4096, 2], P(('grp', 'ep')), parts along dimension 0, may hold values from 0.2 to 1
Outputs:
- mixed: bfloat16 [4096, 1024], P(('grp', 'ep', 'tp')), parts along dimension 0
The draws below stay inside these ranges and needn't reach their ends.
There are 2 independent parts, one for each index of `grp`. The reference program is written for one: setup_inputs(seed, part) draws one part's arguments, and reference() takes and returns one part's arrays. A program takes and returns all parts, laid end to end along the dimension named above; an argument that names none is the same for every part. Nothing has to cross between parts.
Inputs may be any that keep to these rules, and one draw needn't show every extreme that they name: `expert_ids`: A token's 2 experts differ. In the rows of one device (128 tokens, aligned blocks) no expert is named more than 80 times, and in every draw some expert is named exactly 80 times in some device's rows.
All inputs are finite; a program needn't handle non-finite values.
Results may differ from the reference program's by a relative error of at most 0.015.
Values may be sent and summed in bfloat16 or wider, within the bound.
A program may use at most 64 MiB of HBM per device.

```python
import math
import jax
import jax.numpy as jnp
import numpy as np
from jax import lax

D = 1024
FF = 3584
TOP_K = 2
TOK_DEV = 128
EXPERTS = 4
TOKENS = 2048
MOST = 80
N_EP = 4
N_TP = 4


def shard_levels(rng, shape, split, least, high):
    gain = 1.0
    for position, shards_of in split:
        steps = jax.random.uniform(jax.random.fold_in(jax.random.fold_in(rng, 6), position), (shards_of,), jnp.float32, least / len(split), high / len(split))
        gain = gain * jnp.repeat(jnp.exp(steps), shape[position] // shards_of).reshape((-1,) + (1,) * (len(shape) - 1 - position))
    return gain


def deal_out(rng, own, number, rows, count, top, most, skew):
    sequence = jax.random.permutation(rng, count)
    crowded, usual = portions_of(count, rows * top, most, skew, True), portions_of(count, rows * top, most, skew, False)
    places = jnp.arange(count)

    def named(lengths, turn):
        used = int((lengths > 0).sum())
        fixed = max(1, used // 4)
        moved = fixed + (places - fixed + turn * (used - fixed)) % max(1, count - fixed)
        return jnp.zeros((count,), jnp.int32).at[sequence[jnp.where(places < fixed, places, moved)]].set(jnp.asarray(lengths, jnp.int32))

    lengths = jnp.where(number % 4 == 0, named(crowded, number // 4), named(usual, number - number // 4 - 1))
    mixed = jax.random.permutation(jax.random.fold_in(own, 3), count)
    giver, sink = mixed[0:count // 2 * 2:2], mixed[1:count // 2 * 2:2]
    slack = jnp.minimum(lengths[giver] - 1, most - lengths[sink]) // 2
    slack = jnp.where((giver == sequence[0]) | (sink == sequence[0]) | (lengths[sink] == 0), 0, jnp.maximum(slack, 0))
    moved = jax.random.randint(jax.random.fold_in(own, 4), (count // 2,), 0, 1 << 20) % (slack + 1)
    lengths = lengths.at[giver].add(-moved).at[sink].add(moved)
    items = jnp.searchsorted(jnp.cumsum(lengths), jnp.arange(rows * top), side="right").astype(jnp.int32)
    table = items.reshape(top, rows).T
    table = table[jax.random.permutation(jax.random.fold_in(own, 1), rows)]
    turn = jax.random.randint(jax.random.fold_in(own, 2), (rows, 1), 0, top)
    return jnp.take_along_axis(table, (jnp.arange(top)[None, :] + turn) % top, axis=1)


def portions_of(count, total, most, lean, full):
    weights = [(1 << 20) // math.isqrt(grade ** lean) + 1 for grade in range(1, count + 1)]
    largest = most if full else min(most, max(-(-total // count), total * weights[0] // sum(weights)))
    least = 1 if total - largest >= count - 1 else 0
    given, rest = [largest] + [least] * (count - 1), total - largest - least * (count - 1)
    while rest > 0:
        candidates = [i for i in range(1, count) if given[i] < largest] or [i for i in range(1, count) if given[i] < most]
        pool, budget = sum([weights[i] for i in candidates]), rest
        for i in candidates:
            more = min(most - given[i], max(1, budget * weights[i] // pool), rest)
            given[i] = given[i] + more
            rest = rest - more
    return np.array(given)


def centred(rng, extent, spread, bound, shards=(), held_as=jnp.bfloat16):
    result = jax.random.normal(rng, extent, jnp.float32) * spread
    if len(shards) > 0:
        result = shard_levels(rng, extent, shards, -0.22, 0.18) * result
    return jnp.clip(result, min=-bound, max=bound).astype(held_as)


def setup_inputs(seed: int = 0, part: int = 0) -> dict:
    streams_of = jax.random.split(jax.random.key(seed), 8)
    own_keys = jax.random.split(jax.random.fold_in(streams_of[7], part), 8)
    tokens = centred(own_keys[0], (TOKENS, D), 1.0, 6.0, ((0, 16),))
    norm_gain = jnp.clip(1.0 + 0.18 * jax.random.normal(streams_of[1], (D,), jnp.float32), 0.1, 1.9)
    gate_weight = centred(streams_of[2], (EXPERTS, D, FF), D ** -0.5, 0.1875, ((0, 4), (2, 4)))
    up_weight = centred(streams_of[3], (EXPERTS, D, FF), D ** -0.5, 0.1875, ((0, 4), (2, 4)))
    down_weight = centred(streams_of[4], (EXPERTS, FF, D), FF ** -0.5, 0.09375, ((0, 4), (1, 4)))
    expert_ids_keys = jax.random.split(jax.random.fold_in(own_keys[5], 1), TOKENS // TOK_DEV)
    expert_ids_turns = jax.random.permutation(jax.random.fold_in(own_keys[5], 3), TOKENS // TOK_DEV)
    expert_ids = jax.vmap(lambda own, number: deal_out(jax.random.fold_in(own_keys[5], 2), own, number, TOK_DEV, EXPERTS, TOP_K, MOST, 2))(expert_ids_keys, expert_ids_turns).reshape((TOKENS, TOP_K))
    route_weight = jnp.clip(0.2 + 0.8 * jax.random.uniform(own_keys[6], (TOKENS, TOP_K), jnp.float32) ** shard_levels(own_keys[6], (TOKENS, TOP_K), ((0, 4),), -0.2, 0.2), 0.2, 1.0)
    return dict(tokens=tokens, norm_gain=norm_gain, gate_weight=gate_weight, up_weight=up_weight, down_weight=down_weight, expert_ids=expert_ids, route_weight=route_weight)


def norm_rows(tokens, norm_gain):
    values = tokens.astype(jnp.float32)
    scaled = values * lax.rsqrt(lax.optimization_barrier(jnp.mean(values * values, axis=-1, keepdims=True)) + 1e-06)
    return (scaled * norm_gain.astype(jnp.float32)).astype(jnp.bfloat16)

def reference(tokens, norm_gain, gate_weight, up_weight, down_weight, expert_ids, route_weight):
    normed = norm_rows(tokens, norm_gain)
    devices_all = N_EP * N_TP
    cap_rows = devices_all * MOST
    flat_ids = expert_ids.astype(jnp.int32).reshape(devices_all, TOK_DEV * TOP_K)
    onehot = (flat_ids[:, :, None] == jnp.arange(EXPERTS, dtype=jnp.int32)[None, None, :]).astype(jnp.int32)
    before = jnp.cumsum(onehot, axis=1) - onehot
    slots = lax.optimization_barrier(jnp.sum(before * onehot, axis=-1))
    owner = jnp.arange(devices_all, dtype=jnp.int32)[:, None]
    row_index = (flat_ids * cap_rows + owner * MOST + slots).reshape(-1).astype(jnp.int32)
    repeated = jnp.repeat(normed, TOP_K, axis=0)
    buffer = jnp.zeros((EXPERTS * cap_rows, D), jnp.bfloat16).at[row_index].set(repeated)
    buffer = buffer.reshape(EXPERTS, cap_rows, D)
    block = FF // N_TP

    def shard_step(total, shard):
        start = (shard * block).astype(jnp.int32)

        def one_expert(items):
            rows, w_gate, w_up, w_down = items
            gate_part = lax.dynamic_slice_in_dim(w_gate, start, block, 1)
            up_part = lax.dynamic_slice_in_dim(w_up, start, block, 1)
            down_part = lax.dynamic_slice_in_dim(w_down, start, block, 0)
            gate = jnp.dot(rows, gate_part, preferred_element_type=jnp.float32)
            upper = jnp.dot(rows, up_part, preferred_element_type=jnp.float32)
            hidden = (jax.nn.silu(gate) * upper).astype(jnp.bfloat16)
            return jnp.dot(hidden, down_part, preferred_element_type=jnp.float32).astype(jnp.bfloat16)
        pieces = lax.map(one_expert, (buffer, gate_weight, up_weight, down_weight))
        picked = pieces.reshape(EXPERTS * cap_rows, D)[row_index].reshape(TOKENS, TOP_K, D)
        return (total + picked.astype(jnp.float32), None)
    total, _ = lax.scan(shard_step, jnp.zeros((TOKENS, TOP_K, D), jnp.float32), jnp.arange(N_TP, dtype=jnp.int32))
    piece = lax.optimization_barrier(total.astype(jnp.bfloat16))
    weighted = lax.optimization_barrier(jnp.sum(piece.astype(jnp.float32) * route_weight.astype(jnp.float32)[:, :, None], axis=1))
    return weighted.astype(jnp.bfloat16)
```

```python
import functools

import jax
import jax.numpy as jnp
from jax import lax
from jax.experimental import pallas as pl
from jax.experimental.pallas import tpu as pltpu
from jax.sharding import PartitionSpec as P

TOP_K = 2
MESH = pl.DeviceIdType.MESH
VMEM_ROOM = 48 << 20


def norm_rows(tokens, norm_gain):
    values = tokens.astype(jnp.float32)
    scaled = values * lax.rsqrt(jnp.mean(values * values, axis=-1, keepdims=True) + 1e-06)
    return (scaled * norm_gain).astype(jnp.bfloat16)


def expert_hidden(rows, gate_weight, up_weight):
    gate = jnp.einsum("e...d,edf->e...f", rows, gate_weight, preferred_element_type=jnp.float32)
    upper = jnp.einsum("e...d,edf->e...f", rows, up_weight, preferred_element_type=jnp.float32)
    return (jax.nn.silu(gate) * upper).astype(jnp.bfloat16)


def weigh_pieces(summed, weights):
    piece = lax.optimization_barrier(summed.astype(jnp.bfloat16)).astype(jnp.float32)
    total = piece[:, 0] * weights[:, 0:1]
    total = total + piece[:, 1] * weights[:, 1:2]
    return total.astype(jnp.bfloat16)


def plain_body(tokens, norm_gain, gate_weight, up_weight, down_weight, expert_ids, route_weight):
    tok_rows = tokens.shape[0]
    width = tokens.shape[1]
    local_experts = gate_weight.shape[0]
    inner = gate_weight.shape[2]
    n_tp = lax.axis_size("tp")
    n_ep = lax.axis_size("ep")
    experts = n_ep * local_experts
    most = max(2, tok_rows * TOP_K * 5 // (4 * experts))
    normed = norm_rows(tokens, norm_gain)
    flat_ids = expert_ids.reshape(n_tp, tok_rows * TOP_K)
    onehot = (flat_ids[:, :, None] == jnp.arange(experts, dtype=jnp.int32)[None, None, :]).astype(
        jnp.int32
    )
    before = jnp.cumsum(onehot, axis=1) - onehot
    slots = jnp.sum(before * onehot, axis=-1)
    owner = jnp.arange(n_tp, dtype=jnp.int32)[:, None]
    row_index = (flat_ids * (n_tp * most) + owner * most + slots).reshape(-1)
    mine = lax.axis_index("tp")
    own_ids = lax.dynamic_slice_in_dim(flat_ids, mine, 1, 0)[0]
    own_slots = lax.dynamic_slice_in_dim(slots, mine, 1, 0)[0]
    own_index = own_ids * most + own_slots
    whole = lax.all_gather(normed, "tp", axis=0, tiled=True)
    sending = (
        jnp.zeros((experts * n_tp * most, width), jnp.bfloat16)
        .at[row_index]
        .set(jnp.repeat(whole, TOP_K, axis=0))
    )
    arrived = lax.all_to_all(
        sending.reshape(experts, n_tp * most, width), "ep", split_axis=0, concat_axis=1, tiled=True
    )
    hidden = expert_hidden(arrived, gate_weight, up_weight)
    by_source = hidden.reshape(local_experts, n_ep, n_tp, most, inner).transpose(2, 0, 1, 3, 4)
    per_device = local_experts * n_ep * most
    product = jnp.einsum(
        "tlnmf,lfd->tlnmd", by_source, down_weight, preferred_element_type=jnp.float32
    )
    own_sums = lax.psum_scatter(
        product.astype(jnp.bfloat16)
        .astype(jnp.float32)
        .reshape(per_device * lax.axis_size("tp"), width)
        .astype(jnp.bfloat16),
        "tp",
        scatter_dimension=0,
        tiled=True,
    )
    own_pieces = own_sums.reshape(local_experts, n_ep, most, width)
    back = lax.all_to_all(own_pieces, "ep", split_axis=1, concat_axis=0, tiled=True)
    picked = back.reshape(experts * most, width)[own_index].reshape(tok_rows, TOP_K, width)
    own_weights = lax.dynamic_slice_in_dim(route_weight, mine * tok_rows, tok_rows, 0)
    return weigh_pieces(picked.astype(jnp.float32), own_weights)


def place(step, n):
    last = step // (2 * n - 1)
    later = (step + 2 * n - 2) // (2 * n - 1)
    dy = ((step + 1) % 2) * later + last
    dz = (1 - dy) * ((step + 1) // 2) + dy * (step // 2 - 1 + last)
    return dy, dz


def step_of(dy, dz, n):
    if dy == 0:
        return 2 * dz - 1 if dz else 0
    return 2 * n - 1 if dz == n - 1 else 2 * dz + 2


def kernel(
    n, tok_ref, gain_ref, share_ref, gate_hbm, up_hbm, down_hbm, out_ref,
    gate, up, down, buf, shares, part, srecv, yrecv, zrecv, tbuf,
    load_sem, w_s, w_r, agz_s, agz_r, agy_s, agy_r, ags_s, ags_r, rss_s, rss_r, rsy_s, rsy_r, rsz_s, rsz_r,
):
    ep = lax.axis_index("ep")
    z = lax.axis_index("tp")
    y, c = ep // 2, ep % 2
    rows, width = tok_ref.shape
    steps = 2 * n
    sib = {"ep": 2 * y + 1 - c}
    across = {"ep": 2 * (1 - y) + c}

    def along(k):
        return {"tp": (z + k) % n}

    def remote(src, dst, send, recv, to):
        return pltpu.make_async_remote_copy(
            src_ref=src, dst_ref=dst, send_sem=send, recv_sem=recv, device_id=to, device_id_type=MESH
        )

    loads = [
        pltpu.make_async_copy(src.at[0], dst, load_sem.at[i])
        for i, (src, dst) in enumerate(((gate_hbm, gate), (up_hbm, up), (down_hbm, down)))
    ]
    for load in loads:
        load.start()

    barrier = pltpu.get_barrier_semaphore()
    for k in range(1, 4):
        pl.semaphore_signal(barrier, inc=1, device_id={"ep": (ep + k) % 4}, device_id_type=MESH)
    for k in range(1, n):
        pl.semaphore_signal(barrier, inc=1, device_id=along(k), device_id_type=MESH)
    buf[z, y, c] = norm_rows(tok_ref[...], gain_ref[...])
    pl.semaphore_wait(barrier, 3 + n - 1)

    def ag_sib(step):
        dy, dz = place(step, n)
        yb, zb = (y + dy) % 2, (z + dz) % n
        return remote(buf.at[zb, yb, c], buf.at[zb, yb, c], ags_s.at[step], ags_r.at[step], sib)

    def ag_y(dz):
        zb = (z + dz) % n
        return remote(buf.at[zb, y, c], buf.at[zb, y, c], agy_s.at[dz], agy_r.at[dz], across)

    def ag_z(k):
        return remote(buf.at[z, y, c], buf.at[z, y, c], agz_s.at[k], agz_r.at[n - k], along(k))

    def share(k):
        to = (ep + k) % 4
        return remote(share_ref.at[to], shares.at[ep], w_s.at[k], w_r.at[4 - k], {"ep": to})

    def rs_sib(step):
        return remote(part.at[step, 1 - c], srecv.at[step], rss_s.at[step], rss_r.at[step], sib)

    def rs_y(dz, step):
        return remote(part.at[step, c], yrecv.at[dz], rsy_s.at[dz], rsy_r.at[dz], across)

    def rs_z(dz):
        return remote(tbuf.at[dz - 1], zrecv.at[n - dz - 1], rsz_s.at[dz], rsz_r.at[n - dz], along(dz))

    ag_y(0).start()
    for k in range(1, n):
        ag_z(k).start()
    for k in range(1, 4):
        share(k).start()
    shares[ep] = share_ref[ep]
    for k in range(1, 4):
        remote(share_ref.at[0], shares.at[(ep + k) % 4], w_s.at[k], w_r.at[k], sib).wait_recv()
    for load in loads:
        load.wait()

    def arrive(step):
        dy, dz = place(step, n)
        yb, zb = (y + dy) % 2, (z + dz) % n
        here = buf.at[zb, yb, c]

        @pl.when(dy == 1)
        def _():
            remote(here, here, agy_s.at[dz], agy_r.at[dz], across).wait_recv()

        @pl.when((dy == 0) & (dz > 0))
        def _():
            remote(here, here, agz_s.at[dz], agz_r.at[dz], sib).wait_recv()
            ag_y(dz).start()

        ag_sib(step).start()

    def combine(step):
        dy, dz = place(step, n)
        rs_sib(step).wait_recv()
        part[step, c] = (part[step, c].astype(jnp.float32) + srecv[step].astype(jnp.float32)).astype(jnp.bfloat16)

        @pl.when((dy == 1) & (dz > 0))
        def _():
            rs_y(dz, step).start()

    def column(row):
        return jnp.transpose(jnp.broadcast_to(row, (rows, rows)))[:, :1]

    def one(step, carry):
        dy, dz = place(step, n)
        yb, zb = (y + dy) % 2, (z + dz) % n
        arrive(step)
        theirs = buf.at[zb, yb, 1 - c]
        remote(theirs, theirs, ags_s.at[step], ags_r.at[step], sib).wait_recv()
        x = buf[zb, yb].reshape(2 * rows, width)
        g = jnp.dot(x, gate[...], preferred_element_type=jnp.float32)
        u = jnp.dot(x, up[...], preferred_element_type=jnp.float32)
        hidden = (jax.nn.silu(g) * u).astype(jnp.bfloat16)
        product = jnp.dot(hidden, down[...], preferred_element_type=jnp.float32)
        for half in range(2):
            w = column(shares[2 * yb + half, pl.ds(zb, 1), :])
            part[step, half] = (product[half * rows : (half + 1) * rows] * w).astype(jnp.bfloat16)
        rs_sib(step).start()

        @pl.when(step > 0)
        def _():
            combine(step - 1)

        return carry

    lax.fori_loop(0, steps, one, 0)
    combine(steps - 1)
    rs_y(0, step_of(1, 0, n)).start()

    def total(dz):
        landed = yrecv.at[dz]
        remote(landed, landed, rsy_s.at[dz], rsy_r.at[dz], across).wait_recv()
        return part[step_of(0, dz, n), c].astype(jnp.float32) + yrecv[dz].astype(jnp.float32)

    for dz in range(1, n):
        tbuf[dz - 1] = total(dz).astype(jnp.bfloat16)
        rs_z(dz).start()
    result = total(0)
    for dz in range(1, n):
        landed = zrecv.at[dz - 1]
        remote(landed, landed, rsz_s.at[dz], rsz_r.at[dz], sib).wait_recv()
        result = result + zrecv[dz - 1].astype(jnp.float32)
    out_ref[...] = result.astype(out_ref.dtype)

    for k in range(1, 4):
        share(k).wait_send()
    for k in range(1, n):
        ag_z(k).wait_send()
        rs_z(k).wait_send()
    for dz in range(n):
        ag_y(dz).wait_send()
        rs_y(dz, step_of(1, dz, n)).wait_send()
    for step in range(steps):
        ag_sib(step).wait_send()
        rs_sib(step).wait_send()


def kernel_bytes(n, rows, width, inner):
    blocks = n * 4 + 2 * n * 2 + 2 * n + n + 2 * (n - 1) + 8
    return 2 * width * (3 * inner + blocks * rows) + 16 * rows * (width + 2 * inner)


def fused_body(tokens, norm_gain, gate_weight, up_weight, down_weight, expert_ids, route_weight):
    rows, width = tokens.shape
    inner = gate_weight.shape[2]
    n = lax.axis_size("tp")
    experts = lax.axis_size("ep")
    named = expert_ids[None, :, :] == jnp.arange(experts, dtype=jnp.int32)[:, None, None]
    share = jnp.sum(jnp.where(named, route_weight[None, :, :], 0.0), axis=-1).reshape(experts, n, rows)
    vmem = pl.BlockSpec(memory_space=pltpu.VMEM)
    anywhere = pl.BlockSpec(memory_space=pl.ANY)
    dma = pltpu.SemaphoreType.DMA
    bf16 = jnp.bfloat16
    return pl.pallas_call(
        functools.partial(kernel, n),
        out_shape=jax.ShapeDtypeStruct((rows, width), bf16),
        in_specs=[vmem] * 3 + [anywhere] * 3,
        out_specs=vmem,
        scratch_shapes=[
            pltpu.VMEM((width, inner), bf16),
            pltpu.VMEM((width, inner), bf16),
            pltpu.VMEM((inner, width), bf16),
            pltpu.VMEM((n, 2, 2, rows, width), bf16),
            pltpu.VMEM((experts, n, rows), jnp.float32),
            pltpu.VMEM((2 * n, 2, rows, width), bf16),
            pltpu.VMEM((2 * n, rows, width), bf16),
            pltpu.VMEM((n, rows, width), bf16),
            pltpu.VMEM((n - 1, rows, width), bf16),
            pltpu.VMEM((n - 1, rows, width), bf16),
            dma((3,)),
        ]
        + [dma((4,))] * 2
        + [dma((n,))] * 4
        + [dma((2 * n,))] * 4
        + [dma((n,))] * 4,
        compiler_params=pltpu.CompilerParams(
            collective_id=0, has_side_effects=True, vmem_limit_bytes=VMEM_ROOM
        ),
    )(tokens, norm_gain.reshape(1, width), share, gate_weight, up_weight, down_weight)


def body(tokens, norm_gain, gate_weight, up_weight, down_weight, expert_ids, route_weight):
    rows, width = tokens.shape
    inner = gate_weight.shape[2]
    n = lax.axis_size("tp")
    fits = kernel_bytes(n, rows, width, inner) <= VMEM_ROOM
    chosen = plain_body
    if lax.axis_size("ep") == 4 and gate_weight.shape[0] == 1 and n > 1 and fits:
        chosen = fused_body
    return chosen(tokens, norm_gain, gate_weight, up_weight, down_weight, expert_ids, route_weight)


def solution(mesh):
    placed = (
        P(("grp", "ep", "tp"), None),
        P(),
        P("ep", None, "tp"),
        P("ep", None, "tp"),
        P("ep", "tp", None),
        P(("grp", "ep"), None),
        P(("grp", "ep"), None),
    )
    return jax.shard_map(
        body, mesh=mesh, in_specs=placed, out_specs=P(("grp", "ep", "tp"), None), check_vma=False
    )
```

```python
import functools

import jax
import jax.numpy as jnp
from jax import lax
from jax.experimental import pallas as pl
from jax.experimental.pallas import tpu as pltpu
from jax.sharding import PartitionSpec as P

TOP_K = 2
MESH = pl.DeviceIdType.MESH
VMEM_ROOM = 60 << 20


def norm_rows(tokens, norm_gain):
    values = tokens.astype(jnp.float32)
    scaled = values * lax.rsqrt(jnp.mean(values * values, axis=-1, keepdims=True) + 1e-06)
    return (scaled * norm_gain).astype(jnp.bfloat16)


def expert_hidden(rows, gate_weight, up_weight):
    gate = jnp.einsum("e...d,edf->e...f", rows, gate_weight, preferred_element_type=jnp.float32)
    upper = jnp.einsum("e...d,edf->e...f", rows, up_weight, preferred_element_type=jnp.float32)
    return (jax.nn.silu(gate) * upper).astype(jnp.bfloat16)


def weigh_pieces(summed, weights):
    piece = lax.optimization_barrier(summed.astype(jnp.bfloat16)).astype(jnp.float32)
    total = piece[:, 0] * weights[:, 0:1]
    total = total + piece[:, 1] * weights[:, 1:2]
    return total.astype(jnp.bfloat16)


def plain_body(tokens, norm_gain, gate_weight, up_weight, down_weight, expert_ids, route_weight):
    tok_rows = tokens.shape[0]
    width = tokens.shape[1]
    local_experts = gate_weight.shape[0]
    inner = gate_weight.shape[2]
    n_tp = lax.axis_size("tp")
    n_ep = lax.axis_size("ep")
    experts = n_ep * local_experts
    most = max(2, tok_rows * TOP_K * 5 // (4 * experts))
    normed = norm_rows(tokens, norm_gain)
    flat_ids = expert_ids.reshape(n_tp, tok_rows * TOP_K)
    onehot = (flat_ids[:, :, None] == jnp.arange(experts, dtype=jnp.int32)[None, None, :]).astype(
        jnp.int32
    )
    before = jnp.cumsum(onehot, axis=1) - onehot
    slots = jnp.sum(before * onehot, axis=-1)
    owner = jnp.arange(n_tp, dtype=jnp.int32)[:, None]
    row_index = (flat_ids * (n_tp * most) + owner * most + slots).reshape(-1)
    mine = lax.axis_index("tp")
    own_ids = lax.dynamic_slice_in_dim(flat_ids, mine, 1, 0)[0]
    own_slots = lax.dynamic_slice_in_dim(slots, mine, 1, 0)[0]
    own_index = own_ids * most + own_slots
    whole = lax.all_gather(normed, "tp", axis=0, tiled=True)
    sending = (
        jnp.zeros((experts * n_tp * most, width), jnp.bfloat16)
        .at[row_index]
        .set(jnp.repeat(whole, TOP_K, axis=0))
    )
    arrived = lax.all_to_all(
        sending.reshape(experts, n_tp * most, width), "ep", split_axis=0, concat_axis=1, tiled=True
    )
    hidden = expert_hidden(arrived, gate_weight, up_weight)
    by_source = hidden.reshape(local_experts, n_ep, n_tp, most, inner).transpose(2, 0, 1, 3, 4)
    per_device = local_experts * n_ep * most
    product = jnp.einsum(
        "tlnmf,lfd->tlnmd", by_source, down_weight, preferred_element_type=jnp.float32
    )
    own_sums = lax.psum_scatter(
        product.astype(jnp.bfloat16)
        .astype(jnp.float32)
        .reshape(per_device * lax.axis_size("tp"), width)
        .astype(jnp.bfloat16),
        "tp",
        scatter_dimension=0,
        tiled=True,
    )
    own_pieces = own_sums.reshape(local_experts, n_ep, most, width)
    back = lax.all_to_all(own_pieces, "ep", split_axis=1, concat_axis=0, tiled=True)
    picked = back.reshape(experts * most, width)[own_index].reshape(tok_rows, TOP_K, width)
    own_weights = lax.dynamic_slice_in_dim(route_weight, mine * tok_rows, tok_rows, 0)
    return weigh_pieces(picked.astype(jnp.float32), own_weights)


def place(step, n):
    last = step // (2 * n - 1)
    later = (step + 2 * n - 2) // (2 * n - 1)
    dy = ((step + 1) % 2) * later + last
    dz = (1 - dy) * ((step + 1) // 2) + dy * (step // 2 - 1 + last)
    return dy, dz


def step_of(dy, dz, n):
    if dy == 0:
        return 2 * dz - 1 if dz else 0
    return 2 * n - 1 if dz == n - 1 else 2 * dz + 2


def kernel(
    n, tok_ref, gain_ref, share_ref, gate_hbm, up_hbm, down_hbm, out_ref,
    gate, up, down, buf, shares, part, srecv, yrecv, zrecv, tbuf,
    load_sem, w_s, w_r, agz_s, agz_r, agy_s, agy_r, ags_s, ags_r, rss_s, rss_r, rsy_s, rsy_r, rsz_s, rsz_r,
):
    ep = lax.axis_index("ep")
    z = lax.axis_index("tp")
    y, c = ep // 2, ep % 2
    rows, width = tok_ref.shape
    steps = 2 * n
    sib = {"ep": 2 * y + 1 - c}
    across = {"ep": 2 * (1 - y) + c}

    def along(k):
        return {"tp": (z + k) % n}

    def remote(src, dst, send, recv, to):
        return pltpu.make_async_remote_copy(
            src_ref=src, dst_ref=dst, send_sem=send, recv_sem=recv, device_id=to, device_id_type=MESH
        )

    loads = [
        pltpu.make_async_copy(src.at[0], dst, load_sem.at[i])
        for i, (src, dst) in enumerate(((gate_hbm, gate), (up_hbm, up), (down_hbm, down)))
    ]
    for load in loads:
        load.start()

    barrier = pltpu.get_barrier_semaphore()
    for k in range(1, 4):
        pl.semaphore_signal(barrier, inc=1, device_id={"ep": (ep + k) % 4}, device_id_type=MESH)
    for k in range(1, n):
        pl.semaphore_signal(barrier, inc=1, device_id=along(k), device_id_type=MESH)
    buf[z, y, c] = norm_rows(tok_ref[...], gain_ref[...])
    pl.semaphore_wait(barrier, 3 + n - 1)

    def ag_sib(step):
        dy, dz = place(step, n)
        yb, zb = (y + dy) % 2, (z + dz) % n
        return remote(buf.at[zb, yb, c], buf.at[zb, yb, c], ags_s.at[step], ags_r.at[step], sib)

    def ag_y(dz):
        zb = (z + dz) % n
        return remote(buf.at[zb, y, c], buf.at[zb, y, c], agy_s.at[dz], agy_r.at[dz], across)

    def ag_z(k):
        return remote(buf.at[z, y, c], buf.at[z, y, c], agz_s.at[k], agz_r.at[n - k], along(k))

    def share(k):
        to = (ep + k) % 4
        return remote(share_ref.at[to], shares.at[ep], w_s.at[k], w_r.at[4 - k], {"ep": to})

    def rs_sib(step):
        return remote(part.at[step, 1 - c], srecv.at[step], rss_s.at[step], rss_r.at[step], sib)

    def rs_y(dz, step):
        return remote(part.at[step, c], yrecv.at[dz], rsy_s.at[dz], rsy_r.at[dz], across)

    def rs_z(dz):
        return remote(tbuf.at[dz - 1], zrecv.at[n - dz - 1], rsz_s.at[dz], rsz_r.at[n - dz], along(dz))

    ag_y(0).start()
    for k in reversed(range(1, n)):
        ag_z(k).start()
    for k in range(1, 4):
        share(k).start()
    shares[ep] = share_ref[ep]
    for k in range(1, 4):
        remote(share_ref.at[0], shares.at[(ep + k) % 4], w_s.at[k], w_r.at[k], sib).wait_recv()
    for load in loads:
        load.wait()

    def arrive(step):
        dy, dz = place(step, n)
        yb, zb = (y + dy) % 2, (z + dz) % n
        here = buf.at[zb, yb, c]

        @pl.when(dy == 1)
        def _():
            remote(here, here, agy_s.at[dz], agy_r.at[dz], across).wait_recv()

        @pl.when((dy == 0) & (dz > 0))
        def _():
            remote(here, here, agz_s.at[dz], agz_r.at[dz], sib).wait_recv()
            ag_y(dz).start()

        ag_sib(step).start()

    def combine(step):
        dy, dz = place(step, n)
        rs_sib(step).wait_recv()
        part[step, c] = (part[step, c].astype(jnp.float32) + srecv[step].astype(jnp.float32)).astype(jnp.bfloat16)

        @pl.when((dy == 1) & (dz > 0))
        def _():
            rs_y(dz, step).start()

    def column(row):
        return jnp.transpose(jnp.broadcast_to(row, (rows, rows)))[:, :1]

    def one(step, carry):
        dy, dz = place(step, n)
        yb, zb = (y + dy) % 2, (z + dz) % n
        arrive(step)
        theirs = buf.at[zb, yb, 1 - c]
        remote(theirs, theirs, ags_s.at[step], ags_r.at[step], sib).wait_recv()
        x = buf[zb, yb].reshape(2 * rows, width)
        g = jnp.dot(x, gate[...], preferred_element_type=jnp.float32)
        u = jnp.dot(x, up[...], preferred_element_type=jnp.float32)
        hidden = (jax.nn.silu(g) * u).astype(jnp.bfloat16)
        product = jnp.dot(hidden, down[...], preferred_element_type=jnp.float32)
        for half in range(2):
            w = column(shares[2 * yb + half, pl.ds(zb, 1), :])
            part[step, half] = (product[half * rows : (half + 1) * rows] * w).astype(jnp.bfloat16)
        rs_sib(step).start()

        @pl.when(step > 0)
        def _():
            combine(step - 1)

        return carry

    lax.fori_loop(0, steps, one, 0)
    combine(steps - 1)
    rs_y(0, step_of(1, 0, n)).start()

    def total(dz):
        landed = yrecv.at[dz]
        remote(landed, landed, rsy_s.at[dz], rsy_r.at[dz], across).wait_recv()
        return part[step_of(0, dz, n), c].astype(jnp.float32) + yrecv[dz].astype(jnp.float32)

    for dz in range(1, n):
        tbuf[dz - 1] = total(dz).astype(jnp.bfloat16)
        rs_z(dz).start()
    result = total(0)
    for dz in range(1, n):
        landed = zrecv.at[dz - 1]
        remote(landed, landed, rsz_s.at[dz], rsz_r.at[dz], sib).wait_recv()
        result = result + zrecv[dz - 1].astype(jnp.float32)
    out_ref[...] = result.astype(out_ref.dtype)

    for k in range(1, 4):
        share(k).wait_send()
    for k in range(1, n):
        ag_z(k).wait_send()
        rs_z(k).wait_send()
    for dz in range(n):
        ag_y(dz).wait_send()
        rs_y(dz, step_of(1, dz, n)).wait_send()
    for step in range(steps):
        ag_sib(step).wait_send()
        rs_sib(step).wait_send()


def kernel_bytes(n, rows, width, inner):
    blocks = n * 4 + 2 * n * 2 + 2 * n + n + 2 * (n - 1) + 8
    return 2 * width * (3 * inner + blocks * rows) + 16 * rows * (width + 2 * inner)


def fused_body(tokens, norm_gain, gate_weight, up_weight, down_weight, expert_ids, route_weight):
    rows, width = tokens.shape
    inner = gate_weight.shape[2]
    n = lax.axis_size("tp")
    experts = lax.axis_size("ep")
    named = expert_ids[None, :, :] == jnp.arange(experts, dtype=jnp.int32)[:, None, None]
    share = jnp.sum(jnp.where(named, route_weight[None, :, :], 0.0), axis=-1).reshape(experts, n, rows)
    vmem = pl.BlockSpec(memory_space=pltpu.VMEM)
    anywhere = pl.BlockSpec(memory_space=pl.ANY)
    dma = pltpu.SemaphoreType.DMA
    bf16 = jnp.bfloat16
    return pl.pallas_call(
        functools.partial(kernel, n),
        out_shape=jax.ShapeDtypeStruct((rows, width), bf16),
        in_specs=[vmem] * 3 + [anywhere] * 3,
        out_specs=vmem,
        scratch_shapes=[
            pltpu.VMEM((width, inner), bf16),
            pltpu.VMEM((width, inner), bf16),
            pltpu.VMEM((inner, width), bf16),
            pltpu.VMEM((n, 2, 2, rows, width), bf16),
            pltpu.VMEM((experts, n, rows), jnp.float32),
            pltpu.VMEM((2 * n, 2, rows, width), bf16),
            pltpu.VMEM((2 * n, rows, width), bf16),
            pltpu.VMEM((n, rows, width), bf16),
            pltpu.VMEM((n - 1, rows, width), bf16),
            pltpu.VMEM((n - 1, rows, width), bf16),
            dma((3,)),
        ]
        + [dma((4,))] * 2
        + [dma((n,))] * 4
        + [dma((2 * n,))] * 4
        + [dma((n,))] * 4,
        compiler_params=pltpu.CompilerParams(
            collective_id=0, has_side_effects=True, vmem_limit_bytes=VMEM_ROOM
        ),
    )(tokens, norm_gain.reshape(1, width), share, gate_weight, up_weight, down_weight)


def body(tokens, norm_gain, gate_weight, up_weight, down_weight, expert_ids, route_weight):
    rows, width = tokens.shape
    inner = gate_weight.shape[2]
    n = lax.axis_size("tp")
    fits = kernel_bytes(n, rows, width, inner) <= VMEM_ROOM
    chosen = plain_body
    if lax.axis_size("ep") == 4 and gate_weight.shape[0] == 1 and n > 1 and fits:
        chosen = fused_body
    return chosen(tokens, norm_gain, gate_weight, up_weight, down_weight, expert_ids, route_weight)


def solution(mesh):
    placed = (
        P(("grp", "ep", "tp"), None),
        P(),
        P("ep", None, "tp"),
        P("ep", None, "tp"),
        P("ep", "tp", None),
        P(("grp", "ep"), None),
        P(("grp", "ep"), None),
    )
    return jax.shard_map(
        body, mesh=mesh, in_specs=placed, out_specs=P(("grp", "ep", "tp"), None), check_vma=False
    )
```
